32 devices in a mesh: sp: 8 (over z, x), tp: 4 (over y, core).
Axes of the slice: x: 2, y: 2, z: 4, core: 2. Of those that a mesh axis runs over, the one named last changes fastest.
Arguments:
- cotangent: bfloat16 [2048, 2048], P('sp', 'tp'), may hold values from -6 to 6
- moe_input: bfloat16 [2048, 2048], P('sp', 'tp'), may hold values from -6 to 6
- routes: int32 [2048, 2], P('sp'), may hold values from 0 to 7, all different within a row; in each aligned block of 256 rows (0 to 255, 256 to 511, ...) at most 96 rows name the same one
- gates: float32 [2048, 2], P('sp'), may hold values from 0.1 to 1
- w_gate: bfloat16 [8, 2048, 2048], P('sp', None, 'tp'), may hold values from -0.125 to 0.125
- w_up: bfloat16 [8, 2048, 2048], P('sp', None, 'tp'), may hold values from -0.125 to 0.125
- w_down: bfloat16 [8, 2048, 2048], P('sp', 'tp'), may hold values from -0.125 to 0.125
- out_proj: bfloat16 [1024, 2048], P('tp'), may hold values from -0.1875 to 0.1875
- conv_in: bfloat16 [1024, 2048], P('tp', 'sp'), may hold values from -6 to 6
- branch: bfloat16 [1024, 2048], P('tp', 'sp'), may hold values from -6 to 6
- state_before: float32 [1024, 2048], P('tp', 'sp'), may hold values from -6 to 6
- state_after: float32 [1024, 2048], P('tp', 'sp'), may hold values from -6 to 6
- jump: float32 [1024, 2048], P('tp', 'sp'), may hold values from -2 to 0, as said below
- recur_weight: bfloat16 [2, 16, 64, 64], P(None, 'tp'), may hold values from -0.75 to 0.75
- input_weight: bfloat16 [2, 16, 64, 64], P(None, 'tp'), may hold values from -0.75 to 0.75
- lam: float32 [2, 1024], P(None, 'tp')
Outputs:
- gate_grad: bfloat16 [8, 2048, 2048], P('sp', None, 'tp')
- up_grad: bfloat16 [8, 2048, 2048], P('sp', None, 'tp')
- down_grad: bfloat16 [8, 2048, 2048], P('sp', 'tp')
- residual_grad: bfloat16 [2048, 2048], P('sp', 'tp')
- out_proj_grad: float32 [1024, 2048], P('tp', 'sp')
- conv_grad: float32 [1024, 2048], P('tp', 'sp')
- branch_grad: float32 [1024, 2048], P('tp', 'sp')
The draws below stay inside these ranges and needn't reach their ends.
Inputs may be any that keep to these rules, and one draw needn't show every extreme that they name: `routes`: each token names 2 different experts. Among the tokens of one index of sp (aligned blocks of 256 rows) no expert is named more than 96 times, a bound that some block reaches. `jump`: every entry is at most -1 / 20480.
All inputs are finite; a program needn't handle non-finite values.
Results may differ from the reference program's by a relative error of at most 0.02.
Values may be sent and summed in bfloat16 or wider, within the bound.
A program may use at most 128 MiB of HBM per device.

```python
import math
import jax
import jax.numpy as jnp
import numpy as np
from jax import lax

D = 2048
RECURRENT_WIDTH = 1024
BW = 64
BLOCKS = 16
FFE = 2048
TOP = 2
TOK_DEV = 256
EXPERTS = 8
SEQUENCE_TOKENS = 2048
CAP = 96
N_SP = 8
N_TP = 4


def draw_lam(key, part):
    k_fast, k_span, k_slow = jax.random.split(jax.random.fold_in(key, 11), 3)
    fast_share = 0.5
    is_fast = jax.random.uniform(k_fast, (2, RECURRENT_WIDTH), jnp.float32) < fast_share
    fast_len = jax.random.uniform(k_span, (2, RECURRENT_WIDTH), jnp.float32, 30.0, 100.0)
    slow_len = SEQUENCE_TOKENS * jax.random.uniform(k_slow, (2, RECURRENT_WIDTH), jnp.float32, 1.0, 2.0)
    length = jnp.where(is_fast, fast_len, slow_len)
    step_rate = 2.0 / (8.0 * length)
    return -jnp.log(jnp.expm1(step_rate))


def draw_jump(key, part):
    folded = jax.random.fold_in(key, 23)
    k_rate, k_cell, random_location, random_extent = jax.random.split(folded, 4)
    blocks = SEQUENCE_TOKENS // TOK_DEV
    block_rate = jnp.exp(jax.random.uniform(k_rate, (blocks,), jnp.float32, math.log(0.2), math.log(0.8)))
    cell_multiplier = jnp.exp(jax.random.uniform(k_cell, (RECURRENT_WIDTH, SEQUENCE_TOKENS), jnp.float32, math.log(0.5), math.log(2.0)))
    token_position = jnp.arange(SEQUENCE_TOKENS, dtype=jnp.int32)
    position_values = jnp.repeat(block_rate, TOK_DEV) / SEQUENCE_TOKENS
    spike_offset = jax.random.randint(random_location, (2,), 0, SEQUENCE_TOKENS)
    spike_mask = ((token_position == spike_offset[0]) | (token_position == spike_offset[1])).astype(jnp.float32)[None, :]
    spike_extent = jnp.log(jax.random.uniform(random_extent, (RECURRENT_WIDTH, 1), jnp.float32, 0.55, 0.8))
    return -position_values[None, :] * cell_multiplier + spike_mask * spike_extent


def spiked(values, own_key, source, target, parts, factor):
    def block_of(position):
        return (jnp.arange(values.shape[position]) // (values.shape[position] // parts)).reshape((-1,) + (1,) * (values.ndim - 1 - position))

    first = jax.random.permutation(own_key, parts)[block_of(target)]
    second = (block_of(target) + parts // 2) % parts
    return jnp.where((block_of(source) == first) | (block_of(source) == second), factor * values, values)


def levels(rng, extent, cuts, least, high):
    loudness = 1.0
    for dim, parts in cuts:
        steps = jax.random.uniform(jax.random.fold_in(jax.random.fold_in(rng, 6), dim), (parts,), jnp.float32, least / len(cuts), high / len(cuts))
        loudness = loudness * jnp.repeat(jnp.exp(steps), extent[dim] // parts).reshape((-1,) + (1,) * (len(extent) - 1 - dim))
    return loudness


def assign_block(rng, own, number, rows, number_of, top, most, skew):
    sequence = jax.random.permutation(rng, number_of)
    heavy_load, ordinary = load_shares(number_of, rows * top, most, skew, True), load_shares(number_of, rows * top, most, skew, False)
    places = jnp.arange(number_of)

    def named(sizes, turn):
        used = int((sizes > 0).sum())
        fixed = max(1, used // 4)
        shifted = fixed + (places - fixed + turn * (used - fixed)) % max(1, number_of - fixed)
        return jnp.zeros((number_of,), jnp.int32).at[sequence[jnp.where(places < fixed, places, shifted)]].set(jnp.asarray(sizes, jnp.int32))

    sizes = jnp.where(number % 4 == 0, named(heavy_load, number // 4), named(ordinary, number - number // 4 - 1))
    mixed = jax.random.permutation(jax.random.fold_in(own, 3), number_of)
    donor, receiver = mixed[0:number_of // 2 * 2:2], mixed[1:number_of // 2 * 2:2]
    margin = jnp.minimum(sizes[donor] - 1, most - sizes[receiver]) // 2
    margin = jnp.where((donor == sequence[0]) | (receiver == sequence[0]) | (sizes[receiver] == 0), 0, jnp.maximum(margin, 0))
    shifted = jax.random.randint(jax.random.fold_in(own, 4), (number_of // 2,), 0, 1 << 20) % (margin + 1)
    sizes = sizes.at[donor].add(-shifted).at[receiver].add(shifted)
    items = jnp.searchsorted(jnp.cumsum(sizes), jnp.arange(rows * top), side="right").astype(jnp.int32)
    listing = items.reshape(top, rows).T
    listing = listing[jax.random.permutation(jax.random.fold_in(own, 1), rows)]
    turn = jax.random.randint(jax.random.fold_in(own, 2), (rows, 1), 0, top)
    return jnp.take_along_axis(listing, (jnp.arange(top)[None, :] + turn) % top, axis=1)


def load_shares(number_of, total, most, lean, full):
    portions = [(1 << 20) // math.isqrt(grade ** lean) + 1 for grade in range(1, number_of + 1)]
    largest = most if full else min(most, max(-(-total // number_of), total * portions[0] // sum(portions)))
    least = 1 if total - largest >= number_of - 1 else 0
    given, surplus = [largest] + [least] * (number_of - 1), total - largest - least * (number_of - 1)
    while surplus > 0:
        free = [i for i in range(1, number_of) if given[i] < largest] or [i for i in range(1, number_of) if given[i] < most]
        whole, remaining = sum([portions[i] for i in free]), surplus
        for i in free:
            extra = min(most - given[i], max(1, remaining * portions[i] // whole), surplus)
            given[i] = given[i] + extra
            surplus = surplus - extra
    return np.array(given)


def bell_draw(rng, shape, spread, limit, cuts=(), kind=jnp.bfloat16):
    array = spread * jax.random.normal(rng, shape, jnp.float32)
    if cuts:
        array = array * levels(rng, shape, cuts, -0.22, 0.18)
    return jnp.clip(array, -limit, limit).astype(kind)


def gaussian_with(key, dims, scale, most, cuts, heavy, kind=jnp.bfloat16):
    array = scale * jax.random.normal(key, dims, jnp.float32)
    if cuts:
        array = array * levels(key, dims, cuts, -0.22, 0.18)
    return jnp.clip(spiked(array, jax.random.fold_in(key, 3), *heavy), -most, most).astype(kind)


def setup_inputs(seed: int = 0) -> dict:
    key_list = jax.random.split(jax.random.key(seed), 17)
    cotangent = gaussian_with(key_list[0], (SEQUENCE_TOKENS, D), 1.0, 6.0, ((0, 8), (1, 4)), (0, 1, 8, 2.0))
    moe_input = bell_draw(key_list[1], (SEQUENCE_TOKENS, D), 1.0, 6.0, ((0, 8), (1, 4)))
    routes_keys = jax.random.split(jax.random.fold_in(key_list[2], 1), SEQUENCE_TOKENS // TOK_DEV)
    routes_turns = jax.random.permutation(jax.random.fold_in(key_list[2], 3), SEQUENCE_TOKENS // TOK_DEV)
    routes = jax.vmap(lambda own, number: assign_block(jax.random.fold_in(key_list[2], 2), own, number, TOK_DEV, EXPERTS, TOP, CAP, 1))(routes_keys, routes_turns).reshape((SEQUENCE_TOKENS, TOP))
    gates = jnp.clip(0.1 + 0.9 * jax.random.uniform(key_list[3], (SEQUENCE_TOKENS, TOP), jnp.float32) ** levels(key_list[3], (SEQUENCE_TOKENS, TOP), ((0, 8),), -0.2, 0.2), 0.1, 1.0)
    w_gate = bell_draw(key_list[4], (EXPERTS, D, FFE), D ** -0.5, 0.125, ((0, 8), (2, 4)))
    w_up = bell_draw(key_list[5], (EXPERTS, D, FFE), D ** -0.5, 0.125, ((0, 8), (2, 4)))
    w_down = bell_draw(key_list[6], (EXPERTS, FFE, D), FFE ** -0.5, 0.125, ((0, 8), (1, 4)))
    out_proj = bell_draw(key_list[7], (RECURRENT_WIDTH, D), RECURRENT_WIDTH ** -0.5, 0.1875, ((0, 4),))
    conv_in = bell_draw(key_list[8], (RECURRENT_WIDTH, SEQUENCE_TOKENS), 1.0, 6.0, ((0, 4), (1, 8)))
    branch = bell_draw(key_list[9], (RECURRENT_WIDTH, SEQUENCE_TOKENS), 1.0, 6.0, ((0, 4), (1, 8)))
    state_before = bell_draw(key_list[10], (RECURRENT_WIDTH, SEQUENCE_TOKENS), 1.0, 6.0, ((0, 4), (1, 8)), jnp.float32)
    state_after = bell_draw(key_list[11], (RECURRENT_WIDTH, SEQUENCE_TOKENS), 1.0, 6.0, ((0, 4), (1, 8)), jnp.float32)
    jump = draw_jump(jax.random.fold_in(key_list[16], 71), 0)
    recur_weight = bell_draw(key_list[13], (2, BLOCKS, BW, BW), BW ** -0.5, 0.75, ((1, 4),))
    input_weight = bell_draw(key_list[14], (2, BLOCKS, BW, BW), BW ** -0.5, 0.75, ((1, 4),))
    lam = draw_lam(jax.random.fold_in(key_list[16], 71), 0)
    return {"cotangent": cotangent, "moe_input": moe_input, "routes": routes, "gates": gates, "w_gate": w_gate, "w_up": w_up, "w_down": w_down, "out_proj": out_proj, "conv_in": conv_in, "branch": branch, "state_before": state_before, "state_after": state_after, "jump": jump, "recur_weight": recur_weight, "input_weight": input_weight, "lam": lam}


decay_scale = 8.0

def silu_parts(pre_act):
    sigmoid_val = jax.nn.sigmoid(pre_act)
    return (pre_act * sigmoid_val, sigmoid_val * (1.0 + pre_act * (1.0 - sigmoid_val)))

def block_map(values, weight):
    return jnp.einsum('nit,nij->njt', values.astype(jnp.float32), weight.astype(jnp.float32), precision=lax.Precision.HIGHEST)

def block_back(gradient, weight):
    return jnp.einsum('njt,nij->nit', gradient, weight.astype(jnp.float32), precision=lax.Precision.HIGHEST)

def gate_values(conv_in, weight_r, weight_i, lam_row, jump):
    channels, length = conv_in.shape
    shaped = conv_in.reshape(weight_r.shape[0], weight_r.shape[1], length)
    recur_gate = jax.nn.sigmoid(block_map(shaped, weight_r).reshape(channels, length))
    inward = jax.nn.sigmoid(block_map(shaped, weight_i).reshape(channels, length))
    speed_row = decay_scale * jax.nn.softplus(-lam_row)[:, None]
    log_decay = -speed_row * recur_gate + jump
    retain = jnp.exp(log_decay)
    root_term = jnp.sqrt(-jnp.expm1(2.0 * log_decay))
    conv_wide = conv_in.astype(jnp.float32)
    return (recur_gate, inward, speed_row, retain, root_term, conv_wide)

def gate_backward(pieces, decay_grad, drive_grad, weight_r, weight_i):
    recur_gate, inward, speed_row, retain, root_term, conv_wide = pieces
    channels, length = conv_wide.shape
    shape_three = (weight_r.shape[0], weight_r.shape[1], length)
    log_grad = decay_grad * retain - drive_grad * inward * conv_wide * retain * retain / root_term
    recur_grad = log_grad * -speed_row * recur_gate * (1.0 - recur_gate)
    inward_grad = drive_grad * root_term * conv_wide * inward * (1.0 - inward)
    direct = drive_grad * root_term * inward
    back_r = block_back(recur_grad.reshape(shape_three), weight_r)
    back_i = block_back(inward_grad.reshape(shape_three), weight_i)
    return direct + (back_r + back_i).reshape(channels, length)

def combine_pair(earlier, latter):
    return (earlier[0] * latter[0], latter[0] * earlier[1] + latter[1])

def expert_terms(routed_rows, routed_grads, gate_weight, up_weight, down_weight):
    pre_gate = jnp.dot(routed_rows, gate_weight, preferred_element_type=jnp.float32)
    pre_up = jnp.dot(routed_rows, up_weight, preferred_element_type=jnp.float32)
    silu_val, silu_slope = silu_parts(pre_gate)
    activation = (silu_val * pre_up).astype(jnp.bfloat16)
    act_grad = jnp.dot(routed_grads, down_weight.T, preferred_element_type=jnp.float32)
    up_hidden = (act_grad * silu_val).astype(jnp.bfloat16)
    gate_hidden = (act_grad * pre_up * silu_slope).astype(jnp.bfloat16)
    down_acc = jnp.dot(activation.T, routed_grads, preferred_element_type=jnp.float32)
    gate_acc = jnp.dot(routed_rows.T, gate_hidden, preferred_element_type=jnp.float32)
    up_acc = jnp.dot(routed_rows.T, up_hidden, preferred_element_type=jnp.float32)
    return (gate_hidden, up_hidden, gate_acc, up_acc, down_acc)

def reference(cotangent, moe_input, routes, gates, w_gate, w_up, w_down, out_proj, conv_in, branch, state_before, state_after, jump, recur_weight, input_weight, lam):
    per_token = routes.shape[1]
    routed = routes.reshape(-1)
    pair_total = routed.shape[0]
    scaled = (cotangent.astype(jnp.float32)[:, None, :] * gates[:, :, None]).astype(jnp.bfloat16)
    scaled = scaled.reshape(pair_total, D)
    copies = jnp.broadcast_to(moe_input[:, None, :], (SEQUENCE_TOKENS, per_token, D)).reshape(pair_total, D)
    zero_row = jnp.zeros((1, D), jnp.bfloat16)
    padded_rows = jnp.concatenate([copies, zero_row], axis=0)
    padded_grads = jnp.concatenate([scaled, zero_row], axis=0)
    buffer_rows = N_SP * CAP
    per_dev = FFE // N_TP

    def one_expert(returned, inputs):
        gate_weight, up_weight, down_weight, expert = inputs
        chosen = jnp.nonzero(routed == expert, size=buffer_rows, fill_value=pair_total)[0].astype(jnp.int32)
        routed_rows = padded_rows[chosen]
        routed_grads = padded_grads[chosen]
        gate_hidden, up_hidden, gate_acc, up_acc, down_acc = expert_terms(routed_rows, routed_grads, gate_weight, up_weight, down_weight)
        split_gate = jnp.einsum('rkf,dkf->krd', gate_hidden.astype(jnp.float32).reshape(buffer_rows, N_TP, per_dev), gate_weight.astype(jnp.float32).reshape(D, N_TP, per_dev), precision=lax.Precision.HIGHEST)
        split_up = jnp.einsum('rkf,dkf->krd', up_hidden.astype(jnp.float32).reshape(buffer_rows, N_TP, per_dev), up_weight.astype(jnp.float32).reshape(D, N_TP, per_dev), precision=lax.Precision.HIGHEST)
        partial_value = (split_gate + split_up).astype(jnp.bfloat16)
        partial_value = lax.optimization_barrier(partial_value)
        row_grad = lax.optimization_barrier(jnp.sum(partial_value.astype(jnp.float32), axis=0)).astype(jnp.bfloat16)
        returned = returned.at[chosen].set(row_grad)
        return (returned, (gate_acc.astype(jnp.bfloat16), up_acc.astype(jnp.bfloat16), down_acc.astype(jnp.bfloat16)))
    start = jnp.zeros((pair_total + 1, D), jnp.bfloat16)
    returned, grads_all = lax.scan(one_expert, start, (w_gate, w_up, w_down, jnp.arange(EXPERTS, dtype=jnp.int32)))
    gate_grad, up_grad, down_grad = grads_all
    backward_rows = returned[:pair_total].reshape(SEQUENCE_TOKENS, per_token, D)
    residual_grad = (cotangent.astype(jnp.float32) + lax.optimization_barrier(jnp.sum(backward_rows.astype(jnp.float32), axis=1))).astype(jnp.bfloat16)
    mix_grad = jnp.dot(out_proj, residual_grad.T, preferred_element_type=jnp.float32)
    pieces_fwd = gate_values(conv_in, recur_weight[0], input_weight[0], lam[0], jump)
    pieces_bwd = gate_values(conv_in, recur_weight[1], input_weight[1], lam[1], jump)
    drive_fwd = pieces_fwd[4] * pieces_fwd[1] * pieces_fwd[5]
    drive_bwd = pieces_bwd[4] * pieces_bwd[1] * pieces_bwd[5]
    lru_out = pieces_fwd[3] * state_before + drive_fwd + pieces_bwd[3] * state_after + drive_bwd
    gelu_val, gelu_back = jax.vjp(jax.nn.gelu, branch.astype(jnp.float32))
    mix = (lru_out * gelu_val).astype(jnp.bfloat16)
    out_proj_grad = jnp.dot(mix, residual_grad, preferred_element_type=jnp.float32)
    lru_grad = mix_grad * gelu_val
    branch_grad = gelu_back(mix_grad * lru_out)[0]
    decay_fwd = pieces_fwd[3]
    decay_bwd = pieces_bwd[3]
    carried_fwd = lax.associative_scan(combine_pair, (decay_fwd, decay_fwd * lru_grad), reverse=True, axis=1)[1]
    carried_bwd = lax.associative_scan(combine_pair, (decay_bwd, decay_bwd * lru_grad), axis=1)[1]
    zeros_col = jnp.zeros((RECURRENT_WIDTH, 1), jnp.float32)
    delta_fwd = lru_grad + jnp.concatenate([carried_fwd[:, 1:], zeros_col], axis=1)
    delta_bwd = lru_grad + jnp.concatenate([zeros_col, carried_bwd[:, :-1]], axis=1)
    conv_grad = gate_backward(pieces_fwd, delta_fwd * state_before, delta_fwd, recur_weight[0], input_weight[0])
    conv_grad = conv_grad + gate_backward(pieces_bwd, delta_bwd * state_after, delta_bwd, recur_weight[1], input_weight[1])
    return (gate_grad, up_grad, down_grad, residual_grad, out_proj_grad, conv_grad, branch_grad)
```

```python
import jax
import jax.numpy as jnp
from jax import lax
from jax.experimental import pallas as pl
from jax.experimental.pallas import tpu as pltpu
from jax.sharding import PartitionSpec as P

decay_scale = 8.0


MESH = pl.DeviceIdType.MESH
VMEM_SPEC = pl.BlockSpec(memory_space=pltpu.VMEM)


def at(sp=None, tp=None):
    sp = lax.axis_index("sp") if sp is None else sp
    tp = lax.axis_index("tp") if tp is None else tp
    return (sp, tp)


def meet(devices):
    barrier = pltpu.get_barrier_semaphore()
    for device in devices:
        pl.semaphore_signal(barrier, inc=1, device_id=device, device_id_type=MESH)
    pl.semaphore_wait(barrier, len(devices))


def remote(source, target, send, recv, device):
    return pltpu.make_async_remote_copy(
        src_ref=source, dst_ref=target, send_sem=send, recv_sem=recv,
        device_id=device, device_id_type=MESH,
    )


def params(collective_id):
    return pltpu.CompilerParams(
        collective_id=collective_id, has_side_effects=True, vmem_limit_bytes=48 * 1024 * 1024
    )


def dispatch(send_rows, send_grads):
    n, tp = lax.axis_size("sp"), lax.axis_size("tp")
    chips = tp // 2
    capacity, width = send_rows.shape[1:]
    groups = min(n, 8)
    span = n // groups

    def kernel(rows_ref, grads_ref, rows_out, grads_out, ss, sr, ps, pr, ys, yr, fs, fr):
        me, place = lax.axis_index("sp"), lax.axis_index("tp")
        chip, core = place // 2, place % 2
        partner = chip * 2 + (1 - core)
        group, inner = me // span, me % span
        pairs = ((rows_ref, rows_out), (grads_ref, grads_out))

        def columns(member):
            return pl.ds(pl.multiple_of(member * width, width), width)

        def peer(step, sign):
            other_group = lax.rem(group + sign * (step // span) + groups, groups)
            return other_group * span + lax.rem(inner + sign * (step % span) + span, span)

        def across(turn, sign):
            return lax.rem(chip + sign * turn + chips, chips) * 2 + core

        meet(
            [at(sp=peer(k, 1)) for k in range(1, n)]
            + [at(tp=partner)]
            + [at(tp=across(t, 1)) for t in range(1, chips)]
        )
        mine = columns(place)
        first = []
        for k in range(1, n):
            to = peer(k, 1)
            for kind, (source, out) in enumerate(pairs):
                copy = remote(
                    source.at[to], out.at[me, :, mine],
                    ss.at[k, kind], sr.at[k, kind], at(sp=to),
                )
                copy.start()
                first.append(copy)
        for source, out in pairs:
            out[me, :, mine] = source[me]
        sent = []
        for g in range(groups):
            base = lax.rem(group - g + groups, groups) * span
            for kind, (source, out) in enumerate(pairs):
                for i in range(span):
                    k = g * span + i
                    if k == 0:
                        continue
                    origin = peer(k, -1)
                    remote(
                        source.at[origin], out.at[origin, :, mine],
                        ss.at[k, kind], sr.at[k, kind], at(sp=origin),
                    ).wait_recv()
                block = out.at[pl.ds(base, span), :, mine]
                if g == 0 and span == 1:
                    block = source.at[pl.ds(base, span)]
                landing = out.at[pl.ds(base, span), :, mine]
                for t in range(1, chips):
                    copy = remote(
                        block, landing, ys.at[g, t, kind], yr.at[g, t, kind], at(tp=across(t, 1))
                    )
                    copy.start()
                    sent.append(copy)
                copy = remote(block, landing, ps.at[g, kind], pr.at[g, kind], at(tp=partner))
                copy.start()
                sent.append(copy)
        for g in range(groups):
            base = lax.rem(group - g + groups, groups) * span
            for kind, (source, out) in enumerate(pairs):
                for t in range(1, chips):
                    block = out.at[pl.ds(base, span), :, columns(across(t, -1))]
                    remote(
                        block, block, ys.at[g, t, kind], yr.at[g, t, kind], at(tp=across(t, -1))
                    ).wait_recv()
                    copy = remote(
                        block, block, fs.at[g, t, kind], fr.at[g, t, kind], at(tp=partner)
                    )
                    copy.start()
                    sent.append(copy)
        for g in range(groups):
            base = lax.rem(group - g + groups, groups) * span
            for kind, (source, out) in enumerate(pairs):
                block = out.at[pl.ds(base, span), :, columns(partner)]
                remote(block, block, ps.at[g, kind], pr.at[g, kind], at(tp=partner)).wait_recv()
                for t in range(1, chips):
                    member = lax.rem(chip - t + chips, chips) * 2 + (1 - core)
                    block = out.at[pl.ds(base, span), :, columns(member)]
                    remote(
                        block, block, fs.at[g, t, kind], fr.at[g, t, kind], at(tp=partner)
                    ).wait_recv()
        for copy in first + sent:
            copy.wait_send()

    full = jax.ShapeDtypeStruct((n, capacity, tp * width), send_rows.dtype)
    dma = pltpu.SemaphoreType.DMA
    sems = [dma((n, 2))] * 2 + [dma((groups, 2))] * 2 + [dma((groups, max(chips, 2), 2))] * 4
    return pl.pallas_call(
        kernel, name="dispatch", out_shape=(full, full),
        in_specs=[VMEM_SPEC] * 2, out_specs=(VMEM_SPEC,) * 2,
        scratch_shapes=sems, compiler_params=params(1),
    )(send_rows, send_grads)


def scatter_sum(partial):
    tp = lax.axis_size("tp")
    chips = tp // 2
    rows, full = partial.shape
    width = full // tp
    strip = 32

    def kernel(part_ref, out_ref, near, total, far, own, ns, nr, ys, yr):
        place = lax.axis_index("tp")
        chip, core = place // 2, place % 2
        partner = chip * 2 + (1 - core)

        def columns(member):
            return pl.ds(pl.multiple_of(member * width, width), width)

        def turned(t, sign):
            return lax.rem(chip + sign * t + chips, chips)

        meet([at(tp=partner)] + [at(tp=turned(t, 1) * 2 + core) for t in range(1, chips)])
        order = list(range(1, chips)) + [0]
        copies = []
        for t in order:
            copy = remote(
                part_ref.at[:, columns(turned(t, 1) * 2 + (1 - core))],
                near.at[t], ns.at[t], nr.at[t], at(tp=partner),
            )
            copy.start()
            copies.append(copy)
        for t, copy in zip(order, copies):
            copy.wait_recv()
            mine = columns(turned(t, 1) * 2 + core)

            @pl.loop(0, rows // strip)
            def _(i):
                where = pl.ds(pl.multiple_of(i * strip, strip), strip)
                value = part_ref[where, mine].astype(jnp.float32) + near[t, where].astype(
                    jnp.float32
                )
                if t == 0:
                    own[where] = value
                else:
                    total[t, where] = value.astype(total.dtype)

        sends = []
        for t in range(1, chips):
            copy = remote(
                total.at[t], far.at[t], ys.at[t], yr.at[t], at(tp=turned(t, 1) * 2 + core)
            )
            copy.start()
            sends.append(copy)
        for copy in sends:
            copy.wait_recv()

        @pl.loop(0, rows // strip)
        def _(i):
            where = pl.ds(pl.multiple_of(i * strip, strip), strip)
            value = own[where]
            for t in range(1, chips):
                value = value + far[t, where].astype(jnp.float32)
            out_ref[where] = value.astype(out_ref.dtype)

        for copy in copies + sends:
            copy.wait_send()

    dma = pltpu.SemaphoreType.DMA
    block = pltpu.VMEM((chips, rows, width), partial.dtype)
    return pl.pallas_call(
        kernel, name="scatter_sum",
        out_shape=jax.ShapeDtypeStruct((rows, width), partial.dtype),
        in_specs=[VMEM_SPEC], out_specs=VMEM_SPEC,
        scratch_shapes=[block, block, block, pltpu.VMEM((rows, width), jnp.float32)]
        + [dma((chips,))] * 4,
        compiler_params=params(2),
    )(partial)


def share(values):
    n = lax.axis_size("sp")

    def kernel(in_ref, out_ref, ss, sr):
        me = lax.axis_index("sp")
        meet([at(sp=lax.rem(me + k, n)) for k in range(1, n)])
        copies = []
        for k in range(1, n):
            copy = remote(
                in_ref, out_ref.at[me], ss.at[k], sr.at[k], at(sp=lax.rem(me + k, n))
            )
            copy.start()
            copies.append(copy)
        out_ref[me] = in_ref[...]
        for k in range(1, n):
            origin = lax.rem(me - k + n, n)
            remote(in_ref, out_ref.at[origin], ss.at[k], sr.at[k], at(sp=origin)).wait_recv()
        for copy in copies:
            copy.wait_send()

    dma = pltpu.SemaphoreType.DMA
    return pl.pallas_call(
        kernel, name="share",
        out_shape=jax.ShapeDtypeStruct((n,) + values.shape, values.dtype),
        in_specs=[VMEM_SPEC], out_specs=VMEM_SPEC,
        scratch_shapes=[dma((n,))] * 2, compiler_params=params(3),
    )(values)


def silu_parts(pre_act):
    sigmoid_val = jax.nn.sigmoid(pre_act)
    return (pre_act * sigmoid_val, sigmoid_val * (1.0 + pre_act * (1.0 - sigmoid_val)))


def block_map(values, weight):
    return jnp.einsum("nit,nij->njt", values, weight, preferred_element_type=jnp.float32)


def block_back(gradient, weight):
    return jnp.einsum(
        "njt,nij->nit", gradient, weight.astype(jnp.float32), precision=lax.Precision.HIGHEST
    )


def gate_values(conv_in, weight_r, weight_i, lam_row, jump):
    channels, length = conv_in.shape
    shaped = conv_in.reshape(weight_r.shape[0], weight_r.shape[1], length)
    recur_gate = jax.nn.sigmoid(block_map(shaped, weight_r).reshape(channels, length))
    inward = jax.nn.sigmoid(block_map(shaped, weight_i).reshape(channels, length))
    speed_row = decay_scale * jax.nn.softplus(-lam_row)[:, None]
    log_decay = -speed_row * recur_gate + jump
    retain = jnp.exp(log_decay)
    root_term = jnp.sqrt(-jnp.expm1(2.0 * log_decay))
    conv_wide = conv_in.astype(jnp.float32)
    return (recur_gate, inward, speed_row, retain, root_term, conv_wide)


def gate_backward(pieces, decay_grad, drive_grad, weight_r, weight_i):
    recur_gate, inward, speed_row, retain, root_term, conv_wide = pieces
    channels, length = conv_wide.shape
    shape_three = (weight_r.shape[0], weight_r.shape[1], length)
    log_grad = decay_grad * retain - drive_grad * inward * conv_wide * retain * retain / root_term
    recur_grad = log_grad * -speed_row * recur_gate * (1.0 - recur_gate)
    inward_grad = drive_grad * root_term * conv_wide * inward * (1.0 - inward)
    direct = drive_grad * root_term * inward
    back_r = block_back(recur_grad.reshape(shape_three), weight_r)
    back_i = block_back(inward_grad.reshape(shape_three), weight_i)
    return direct + (back_r + back_i).reshape(channels, length)


def combine_pair(earlier, latter):
    return (earlier[0] * latter[0], latter[0] * earlier[1] + latter[1])


def expert_pass(full_rows, full_grads, gate_weight, up_weight, down_weight):
    contract_last = (((1,), (1,)), ((), ()))
    contract_first = (((0,), (0,)), ((), ()))
    pre_gate = jnp.dot(full_rows, gate_weight, preferred_element_type=jnp.float32)
    pre_up = jnp.dot(full_rows, up_weight, preferred_element_type=jnp.float32)
    silu_val, silu_slope = silu_parts(pre_gate)
    activation = (silu_val * pre_up).astype(jnp.bfloat16)
    act_grad = lax.dot_general(
        full_grads, down_weight, contract_last, preferred_element_type=jnp.float32
    )
    up_hidden = (act_grad * silu_val).astype(jnp.bfloat16)
    gate_hidden = (act_grad * pre_up * silu_slope).astype(jnp.bfloat16)
    partial_value = lax.dot_general(
        gate_hidden, gate_weight, contract_last, preferred_element_type=jnp.float32
    )
    partial_value = (
        partial_value
        + lax.dot_general(up_hidden, up_weight, contract_last, preferred_element_type=jnp.float32)
    ).astype(jnp.bfloat16)
    gate_acc = lax.dot_general(
        full_rows, gate_hidden, contract_first, preferred_element_type=jnp.float32
    )
    up_acc = lax.dot_general(
        full_rows, up_hidden, contract_first, preferred_element_type=jnp.float32
    )
    down_acc = lax.dot_general(
        activation, full_grads, contract_first, preferred_element_type=jnp.float32
    )
    return (partial_value, (gate_acc, up_acc, down_acc))


def on_device(
    cotangent,
    moe_input,
    routes,
    gates,
    w_gate,
    w_up,
    w_down,
    out_proj,
    conv_in,
    branch,
    state_before,
    state_after,
    jump,
    recur_weight,
    input_weight,
    lam,
):
    tokens_dev, width_dev = cotangent.shape
    per_token = routes.shape[1]
    experts = lax.axis_size("sp")
    capacity = 3 * tokens_dev // experts
    pair_total = tokens_dev * per_token
    routed = routes.reshape(-1)
    onehot = (routed[:, None] == jnp.arange(experts, dtype=jnp.int32)[None, :]).astype(jnp.int32)
    earlier_count = jnp.cumsum(onehot, axis=0) - onehot
    token_position = jnp.sum(earlier_count * onehot, axis=1)
    target = routed * capacity + token_position
    scaled = (cotangent.astype(jnp.float32)[:, None, :] * gates[:, :, None]).astype(jnp.bfloat16)
    scaled = scaled.reshape(pair_total, width_dev)
    copies = jnp.broadcast_to(moe_input[:, None, :], (tokens_dev, per_token, width_dev)).reshape(
        pair_total, width_dev
    )
    blank = jnp.zeros((experts * capacity, width_dev), jnp.bfloat16)
    send_rows = blank.at[target].set(copies).reshape(experts, capacity, width_dev)
    send_grads = blank.at[target].set(scaled).reshape(experts, capacity, width_dev)
    total_rows = experts * capacity
    full_rows, full_grads = dispatch(send_rows, send_grads)
    full_rows = full_rows.reshape(total_rows, -1)
    full_grads = full_grads.reshape(total_rows, -1)
    partial_value, totals = expert_pass(full_rows, full_grads, w_gate[0], w_up[0], w_down[0])
    row_grad = scatter_sum(partial_value)
    gate_grad = totals[0].astype(jnp.bfloat16)[None]
    up_grad = totals[1].astype(jnp.bfloat16)[None]
    down_grad = totals[2].astype(jnp.bfloat16)[None]
    returned = lax.all_to_all(
        row_grad.reshape(experts, capacity, width_dev),
        "sp",
        split_axis=0,
        concat_axis=0,
        tiled=True,
    )
    returned = returned.reshape(experts * capacity, width_dev)[target].reshape(
        tokens_dev, per_token, width_dev
    )
    residual_grad = (
        cotangent.astype(jnp.float32) + jnp.sum(returned.astype(jnp.float32), axis=1)
    ).astype(jnp.bfloat16)
    full_residual = lax.all_gather(residual_grad, "tp", axis=1, tiled=True)
    pieces_fwd = gate_values(conv_in, recur_weight[0], input_weight[0], lam[0], jump)
    pieces_bwd = gate_values(conv_in, recur_weight[1], input_weight[1], lam[1], jump)
    drive_fwd = pieces_fwd[4] * pieces_fwd[1] * pieces_fwd[5]
    drive_bwd = pieces_bwd[4] * pieces_bwd[1] * pieces_bwd[5]
    lru_out = pieces_fwd[3] * state_before + drive_fwd + pieces_bwd[3] * state_after + drive_bwd
    gelu_val, gelu_back = jax.vjp(jax.nn.gelu, branch.astype(jnp.float32))
    mix = (lru_out * gelu_val).astype(jnp.bfloat16)
    proj_part = lax.dot_general(
        full_residual, mix, (((0,), (1,)), ((), ())), preferred_element_type=jnp.float32
    ).astype(jnp.bfloat16)
    proj_part, full_residual = lax.optimization_barrier((proj_part, full_residual))
    proj_rows = lax.psum_scatter(proj_part, "sp", scatter_dimension=0, tiled=True).astype(
        jnp.float32
    )
    out_proj_grad = proj_rows.T
    mix_grad = lax.dot_general(
        out_proj, full_residual, (((1,), (1,)), ((), ())), preferred_element_type=jnp.float32
    )
    lru_grad = mix_grad * gelu_val
    branch_grad = gelu_back(mix_grad * lru_out)[0]
    decay_fwd = pieces_fwd[3]
    decay_bwd = pieces_bwd[3]
    prod_fwd, local_fwd = lax.associative_scan(
        combine_pair, (decay_fwd, decay_fwd * lru_grad), reverse=True, axis=1
    )
    prod_bwd, local_bwd = lax.associative_scan(
        combine_pair, (decay_bwd, decay_bwd * lru_grad), axis=1
    )
    ends = jnp.concatenate([prod_fwd[:, 0], local_fwd[:, 0], prod_bwd[:, -1], local_bwd[:, -1]])
    shared = share(ends[None]).reshape(experts, 4, -1)
    place = lax.axis_index("sp")
    incoming_fwd = jnp.zeros_like(local_fwd[:, 0])
    incoming_bwd = jnp.zeros_like(incoming_fwd)
    for turn in range(experts - 1):
        late = experts - 1 - turn
        incoming_fwd = jnp.where(
            late > place, shared[late, 0] * incoming_fwd + shared[late, 1], incoming_fwd
        )
        incoming_bwd = jnp.where(
            turn < place, shared[turn, 2] * incoming_bwd + shared[turn, 3], incoming_bwd
        )
    carried_fwd = local_fwd + prod_fwd * incoming_fwd[:, None]
    carried_bwd = local_bwd + prod_bwd * incoming_bwd[:, None]
    delta_fwd = lru_grad + jnp.concatenate([carried_fwd[:, 1:], incoming_fwd[:, None]], axis=1)
    delta_bwd = lru_grad + jnp.concatenate([incoming_bwd[:, None], carried_bwd[:, :-1]], axis=1)
    conv_grad = gate_backward(
        pieces_fwd, delta_fwd * state_before, delta_fwd, recur_weight[0], input_weight[0]
    )
    conv_grad = conv_grad + gate_backward(
        pieces_bwd, delta_bwd * state_after, delta_bwd, recur_weight[1], input_weight[1]
    )
    return (gate_grad, up_grad, down_grad, residual_grad, out_proj_grad, conv_grad, branch_grad)


def solution(mesh):
    placed = (
        P("sp", "tp"),
        P("sp", "tp"),
        P("sp", None),
        P("sp", None),
        P("sp", None, "tp"),
        P("sp", None, "tp"),
        P("sp", "tp", None),
        P("tp", None),
        P("tp", "sp"),
        P("tp", "sp"),
        P("tp", "sp"),
        P("tp", "sp"),
        P("tp", "sp"),
        P(None, "tp", None, None),
        P(None, "tp", None, None),
        P(None, "tp"),
    )
    return jax.shard_map(
        on_device,
        mesh=mesh,
        in_specs=placed,
        out_specs=(
            P("sp", None, "tp"),
            P("sp", None, "tp"),
            P("sp", "tp", None),
            P("sp", "tp"),
            P("tp", "sp"),
            P("tp", "sp"),
            P("tp", "sp"),
        ),
        check_vma=False,
    )
```

```python
import jax
import jax.numpy as jnp
from jax import lax
from jax.experimental import pallas as pl
from jax.experimental.pallas import tpu as pltpu
from jax.sharding import PartitionSpec as P

decay_scale = 8.0


MESH = pl.DeviceIdType.MESH
VMEM_SPEC = pl.BlockSpec(memory_space=pltpu.VMEM)


def at(sp=None, tp=None):
    sp = lax.axis_index("sp") if sp is None else sp
    tp = lax.axis_index("tp") if tp is None else tp
    return (sp, tp)


def meet(devices):
    barrier = pltpu.get_barrier_semaphore()
    for device in devices:
        pl.semaphore_signal(barrier, inc=1, device_id=device, device_id_type=MESH)
    pl.semaphore_wait(barrier, len(devices))


def remote(source, target, send, recv, device):
    return pltpu.make_async_remote_copy(
        src_ref=source, dst_ref=target, send_sem=send, recv_sem=recv,
        device_id=device, device_id_type=MESH,
    )


def params(collective_id):
    return pltpu.CompilerParams(
        collective_id=collective_id, has_side_effects=True, vmem_limit_bytes=48 * 1024 * 1024
    )


def dispatch(send_rows, send_grads):
    n, tp = lax.axis_size("sp"), lax.axis_size("tp")
    chips = tp // 2
    capacity, width = send_rows.shape[1:]
    groups = min(n, 8)
    span = n // groups

    def kernel(rows_ref, grads_ref, rows_out, grads_out, ss, sr, ps, pr, ys, yr, fs, fr):
        me, place = lax.axis_index("sp"), lax.axis_index("tp")
        chip, core = place // 2, place % 2
        partner = chip * 2 + (1 - core)
        group, inner = me // span, me % span
        pairs = ((rows_ref, rows_out), (grads_ref, grads_out))

        def columns(member):
            return pl.ds(pl.multiple_of(member * width, width), width)

        def peer(step, sign):
            other_group = lax.rem(group + sign * (step // span) + groups, groups)
            return other_group * span + lax.rem(inner + sign * (step % span) + span, span)

        def across(turn, sign):
            return lax.rem(chip + sign * turn + chips, chips) * 2 + core

        meet(
            [at(sp=peer(k, 1)) for k in range(1, n)]
            + [at(tp=partner)]
            + [at(tp=across(t, 1)) for t in range(1, chips)]
        )
        mine = columns(place)
        first = []
        for k in range(1, n):
            to = peer(k, 1)
            for kind, (source, out) in enumerate(pairs):
                copy = remote(
                    source.at[to], out.at[me, :, mine],
                    ss.at[k, kind], sr.at[k, kind], at(sp=to),
                )
                copy.start()
                first.append(copy)
        for source, out in pairs:
            out[me, :, mine] = source[me]
        sent = []
        for g in range(groups):
            base = lax.rem(group - g + groups, groups) * span
            for kind, (source, out) in enumerate(pairs):
                for i in range(span):
                    k = g * span + i
                    if k == 0:
                        continue
                    origin = peer(k, -1)
                    remote(
                        source.at[origin], out.at[origin, :, mine],
                        ss.at[k, kind], sr.at[k, kind], at(sp=origin),
                    ).wait_recv()
                block = out.at[pl.ds(base, span), :, mine]
                if g == 0 and span == 1:
                    block = source.at[pl.ds(base, span)]
                landing = out.at[pl.ds(base, span), :, mine]
                for t in range(1, chips):
                    copy = remote(
                        block, landing, ys.at[g, t, kind], yr.at[g, t, kind], at(tp=across(t, 1))
                    )
                    copy.start()
                    sent.append(copy)
                copy = remote(block, landing, ps.at[g, kind], pr.at[g, kind], at(tp=partner))
                copy.start()
                sent.append(copy)
        for g in range(groups):
            base = lax.rem(group - g + groups, groups) * span
            for kind, (source, out) in enumerate(pairs):
                for t in range(1, chips):
                    block = out.at[pl.ds(base, span), :, columns(across(t, -1))]
                    remote(
                        block, block, ys.at[g, t, kind], yr.at[g, t, kind], at(tp=across(t, -1))
                    ).wait_recv()
                    copy = remote(
                        block, block, fs.at[g, t, kind], fr.at[g, t, kind], at(tp=partner)
                    )
                    copy.start()
                    sent.append(copy)
        for g in range(groups):
            base = lax.rem(group - g + groups, groups) * span
            for kind, (source, out) in enumerate(pairs):
                block = out.at[pl.ds(base, span), :, columns(partner)]
                remote(block, block, ps.at[g, kind], pr.at[g, kind], at(tp=partner)).wait_recv()
                for t in range(1, chips):
                    member = lax.rem(chip - t + chips, chips) * 2 + (1 - core)
                    block = out.at[pl.ds(base, span), :, columns(member)]
                    remote(
                        block, block, fs.at[g, t, kind], fr.at[g, t, kind], at(tp=partner)
                    ).wait_recv()
        for copy in first + sent:
            copy.wait_send()

    full = jax.ShapeDtypeStruct((n, capacity, tp * width), send_rows.dtype)
    dma = pltpu.SemaphoreType.DMA
    sems = [dma((n, 2))] * 2 + [dma((groups, 2))] * 2 + [dma((groups, max(chips, 2), 2))] * 4
    return pl.pallas_call(
        kernel, name="dispatch", out_shape=(full, full),
        in_specs=[VMEM_SPEC] * 2, out_specs=(VMEM_SPEC,) * 2,
        scratch_shapes=sems, compiler_params=params(1),
    )(send_rows, send_grads)


def scatter_sum(partial):
    tp = lax.axis_size("tp")
    chips = tp // 2
    rows, full = partial.shape
    width = full // tp
    strip = 32

    def kernel(part_ref, out_ref, near, total, far, own, ns, nr, ys, yr):
        place = lax.axis_index("tp")
        chip, core = place // 2, place % 2
        partner = chip * 2 + (1 - core)

        def columns(member):
            return pl.ds(pl.multiple_of(member * width, width), width)

        def turned(t, sign):
            return lax.rem(chip + sign * t + chips, chips)

        meet([at(tp=partner)] + [at(tp=turned(t, 1) * 2 + core) for t in range(1, chips)])
        order = list(range(1, chips)) + [0]
        copies = []
        for t in order:
            copy = remote(
                part_ref.at[:, columns(turned(t, 1) * 2 + (1 - core))],
                near.at[t], ns.at[t], nr.at[t], at(tp=partner),
            )
            copy.start()
            copies.append(copy)
        for t, copy in zip(order, copies):
            copy.wait_recv()
            mine = columns(turned(t, 1) * 2 + core)

            @pl.loop(0, rows // strip)
            def _(i):
                where = pl.ds(pl.multiple_of(i * strip, strip), strip)
                value = part_ref[where, mine].astype(jnp.float32) + near[t, where].astype(
                    jnp.float32
                )
                if t == 0:
                    own[where] = value
                else:
                    total[t, where] = value.astype(total.dtype)

        sends = []
        for t in range(1, chips):
            copy = remote(
                total.at[t], far.at[t], ys.at[t], yr.at[t], at(tp=turned(t, 1) * 2 + core)
            )
            copy.start()
            sends.append(copy)
        for copy in sends:
            copy.wait_recv()

        @pl.loop(0, rows // strip)
        def _(i):
            where = pl.ds(pl.multiple_of(i * strip, strip), strip)
            value = own[where]
            for t in range(1, chips):
                value = value + far[t, where].astype(jnp.float32)
            out_ref[where] = value.astype(out_ref.dtype)

        for copy in copies + sends:
            copy.wait_send()

    dma = pltpu.SemaphoreType.DMA
    block = pltpu.VMEM((chips, rows, width), partial.dtype)
    return pl.pallas_call(
        kernel, name="scatter_sum",
        out_shape=jax.ShapeDtypeStruct((rows, width), partial.dtype),
        in_specs=[VMEM_SPEC], out_specs=VMEM_SPEC,
        scratch_shapes=[block, block, block, pltpu.VMEM((rows, width), jnp.float32)]
        + [dma((chips,))] * 4,
        compiler_params=params(2),
    )(partial)


def share(values):
    n = lax.axis_size("sp")

    def kernel(in_ref, out_ref, ss, sr):
        me = lax.axis_index("sp")
        meet([at(sp=lax.rem(me + k, n)) for k in range(1, n)])
        copies = []
        for k in range(1, n):
            copy = remote(
                in_ref, out_ref.at[me], ss.at[k], sr.at[k], at(sp=lax.rem(me + k, n))
            )
            copy.start()
            copies.append(copy)
        out_ref[me] = in_ref[...]
        for k in range(1, n):
            origin = lax.rem(me - k + n, n)
            remote(in_ref, out_ref.at[origin], ss.at[k], sr.at[k], at(sp=origin)).wait_recv()
        for copy in copies:
            copy.wait_send()

    dma = pltpu.SemaphoreType.DMA
    return pl.pallas_call(
        kernel, name="share",
        out_shape=jax.ShapeDtypeStruct((n,) + values.shape, values.dtype),
        in_specs=[VMEM_SPEC], out_specs=VMEM_SPEC,
        scratch_shapes=[dma((n,))] * 2, compiler_params=params(3),
    )(values)


def silu_parts(pre_act):
    sigmoid_val = jax.nn.sigmoid(pre_act)
    return (pre_act * sigmoid_val, sigmoid_val * (1.0 + pre_act * (1.0 - sigmoid_val)))


def block_map(values, weight):
    return jnp.einsum("nit,nij->njt", values, weight, preferred_element_type=jnp.float32)


def block_back(gradient, weight):
    return jnp.einsum(
        "njt,nij->nit", gradient, weight.astype(jnp.float32), precision=lax.Precision.HIGHEST
    )


def gate_values(conv_in, weight_r, weight_i, lam_row, jump):
    channels, length = conv_in.shape
    shaped = conv_in.reshape(weight_r.shape[0], weight_r.shape[1], length)
    recur_gate = jax.nn.sigmoid(block_map(shaped, weight_r).reshape(channels, length))
    inward = jax.nn.sigmoid(block_map(shaped, weight_i).reshape(channels, length))
    speed_row = decay_scale * jax.nn.softplus(-lam_row)[:, None]
    log_decay = -speed_row * recur_gate + jump
    retain = jnp.exp(log_decay)
    root_term = jnp.sqrt(-jnp.expm1(2.0 * log_decay))
    conv_wide = conv_in.astype(jnp.float32)
    return (recur_gate, inward, speed_row, retain, root_term, conv_wide)


def gate_backward(pieces, decay_grad, drive_grad, weight_r, weight_i):
    recur_gate, inward, speed_row, retain, root_term, conv_wide = pieces
    channels, length = conv_wide.shape
    shape_three = (weight_r.shape[0], weight_r.shape[1], length)
    log_grad = decay_grad * retain - drive_grad * inward * conv_wide * retain * retain / root_term
    recur_grad = log_grad * -speed_row * recur_gate * (1.0 - recur_gate)
    inward_grad = drive_grad * root_term * conv_wide * inward * (1.0 - inward)
    direct = drive_grad * root_term * inward
    back_r = block_back(recur_grad.reshape(shape_three), weight_r)
    back_i = block_back(inward_grad.reshape(shape_three), weight_i)
    return direct + (back_r + back_i).reshape(channels, length)


def combine_pair(earlier, latter):
    return (earlier[0] * latter[0], latter[0] * earlier[1] + latter[1])


def expert_pass(full_rows, full_grads, gate_weight, up_weight, down_weight):
    contract_last = (((1,), (1,)), ((), ()))
    contract_first = (((0,), (0,)), ((), ()))
    pre_gate = jnp.dot(full_rows, gate_weight, preferred_element_type=jnp.float32)
    pre_up = jnp.dot(full_rows, up_weight, preferred_element_type=jnp.float32)
    silu_val, silu_slope = silu_parts(pre_gate)
    activation = (silu_val * pre_up).astype(jnp.bfloat16)
    act_grad = lax.dot_general(
        full_grads, down_weight, contract_last, preferred_element_type=jnp.float32
    )
    up_hidden = (act_grad * silu_val).astype(jnp.bfloat16)
    gate_hidden = (act_grad * pre_up * silu_slope).astype(jnp.bfloat16)
    partial_value = lax.dot_general(
        gate_hidden, gate_weight, contract_last, preferred_element_type=jnp.float32
    )
    partial_value = (
        partial_value
        + lax.dot_general(up_hidden, up_weight, contract_last, preferred_element_type=jnp.float32)
    ).astype(jnp.bfloat16)
    gate_acc = lax.dot_general(
        full_rows, gate_hidden, contract_first, preferred_element_type=jnp.float32
    )
    up_acc = lax.dot_general(
        full_rows, up_hidden, contract_first, preferred_element_type=jnp.float32
    )
    down_acc = lax.dot_general(
        activation, full_grads, contract_first, preferred_element_type=jnp.float32
    )
    return (partial_value, (gate_acc, up_acc, down_acc))


def on_device(
    cotangent,
    moe_input,
    routes,
    gates,
    w_gate,
    w_up,
    w_down,
    out_proj,
    conv_in,
    branch,
    state_before,
    state_after,
    jump,
    recur_weight,
    input_weight,
    lam,
):
    tokens_dev, width_dev = cotangent.shape
    per_token = routes.shape[1]
    experts = lax.axis_size("sp")
    capacity = 3 * tokens_dev // experts
    pair_total = tokens_dev * per_token
    routed = routes.reshape(-1)
    onehot = (routed[:, None] == jnp.arange(experts, dtype=jnp.int32)[None, :]).astype(jnp.int32)
    earlier_count = jnp.cumsum(onehot, axis=0) - onehot
    token_position = jnp.sum(earlier_count * onehot, axis=1)
    target = routed * capacity + token_position
    scaled = (cotangent.astype(jnp.float32)[:, None, :] * gates[:, :, None]).astype(jnp.bfloat16)
    scaled = scaled.reshape(pair_total, width_dev)
    copies = jnp.broadcast_to(moe_input[:, None, :], (tokens_dev, per_token, width_dev)).reshape(
        pair_total, width_dev
    )
    blank = jnp.zeros((experts * capacity, width_dev), jnp.bfloat16)
    send_rows = blank.at[target].set(copies).reshape(experts, capacity, width_dev)
    send_grads = blank.at[target].set(scaled).reshape(experts, capacity, width_dev)
    total_rows = experts * capacity
    full_rows, full_grads = dispatch(send_rows, send_grads)
    full_rows = full_rows.reshape(total_rows, -1)
    full_grads = full_grads.reshape(total_rows, -1)
    partial_value, totals = expert_pass(full_rows, full_grads, w_gate[0], w_up[0], w_down[0])
    row_grad = scatter_sum(partial_value)
    gate_grad = totals[0].astype(jnp.bfloat16)[None]
    up_grad = totals[1].astype(jnp.bfloat16)[None]
    down_grad = totals[2].astype(jnp.bfloat16)[None]
    returned = lax.all_to_all(
        row_grad.reshape(experts, capacity, width_dev),
        "sp",
        split_axis=0,
        concat_axis=0,
        tiled=True,
    )
    returned = returned.reshape(experts * capacity, width_dev)[target].reshape(
        tokens_dev, per_token, width_dev
    )
    residual_grad = (
        cotangent.astype(jnp.float32) + jnp.sum(returned.astype(jnp.float32), axis=1)
    ).astype(jnp.bfloat16)
    full_residual = lax.all_gather(residual_grad, "tp", axis=1, tiled=True)
    pieces_fwd = gate_values(conv_in, recur_weight[0], input_weight[0], lam[0], jump)
    pieces_bwd = gate_values(conv_in, recur_weight[1], input_weight[1], lam[1], jump)
    drive_fwd = pieces_fwd[4] * pieces_fwd[1] * pieces_fwd[5]
    drive_bwd = pieces_bwd[4] * pieces_bwd[1] * pieces_bwd[5]
    lru_out = pieces_fwd[3] * state_before + drive_fwd + pieces_bwd[3] * state_after + drive_bwd
    gelu_val, gelu_back = jax.vjp(jax.nn.gelu, branch.astype(jnp.float32))
    mix = (lru_out * gelu_val).astype(jnp.bfloat16)
    proj_part = lax.dot_general(
        full_residual, mix, (((0,), (1,)), ((), ())), preferred_element_type=jnp.float32
    ).astype(jnp.bfloat16)
    proj_part, full_residual = lax.optimization_barrier((proj_part, full_residual))
    proj_blocks = lax.all_to_all(
        proj_part.reshape(experts, -1, proj_part.shape[1]), "sp", split_axis=0, concat_axis=0, tiled=True
    )
    proj_rows = jnp.sum(proj_blocks.astype(jnp.float32), axis=0)
    out_proj_grad = proj_rows.T
    mix_grad = lax.dot_general(
        out_proj, full_residual, (((1,), (1,)), ((), ())), preferred_element_type=jnp.float32
    )
    lru_grad = mix_grad * gelu_val
    branch_grad = gelu_back(mix_grad * lru_out)[0]
    decay_fwd = pieces_fwd[3]
    decay_bwd = pieces_bwd[3]
    prod_fwd, local_fwd = lax.associative_scan(
        combine_pair, (decay_fwd, decay_fwd * lru_grad), reverse=True, axis=1
    )
    prod_bwd, local_bwd = lax.associative_scan(
        combine_pair, (decay_bwd, decay_bwd * lru_grad), axis=1
    )
    ends = jnp.concatenate([prod_fwd[:, 0], local_fwd[:, 0], prod_bwd[:, -1], local_bwd[:, -1]])
    shared = share(ends[None]).reshape(experts, 4, -1)
    place = lax.axis_index("sp")
    incoming_fwd = jnp.zeros_like(local_fwd[:, 0])
    incoming_bwd = jnp.zeros_like(incoming_fwd)
    for turn in range(experts - 1):
        late = experts - 1 - turn
        incoming_fwd = jnp.where(
            late > place, shared[late, 0] * incoming_fwd + shared[late, 1], incoming_fwd
        )
        incoming_bwd = jnp.where(
            turn < place, shared[turn, 2] * incoming_bwd + shared[turn, 3], incoming_bwd
        )
    carried_fwd = local_fwd + prod_fwd * incoming_fwd[:, None]
    carried_bwd = local_bwd + prod_bwd * incoming_bwd[:, None]
    delta_fwd = lru_grad + jnp.concatenate([carried_fwd[:, 1:], incoming_fwd[:, None]], axis=1)
    delta_bwd = lru_grad + jnp.concatenate([incoming_bwd[:, None], carried_bwd[:, :-1]], axis=1)
    conv_grad = gate_backward(
        pieces_fwd, delta_fwd * state_before, delta_fwd, recur_weight[0], input_weight[0]
    )
    conv_grad = conv_grad + gate_backward(
        pieces_bwd, delta_bwd * state_after, delta_bwd, recur_weight[1], input_weight[1]
    )
    return (gate_grad, up_grad, down_grad, residual_grad, out_proj_grad, conv_grad, branch_grad)


def solution(mesh):
    placed = (
        P("sp", "tp"),
        P("sp", "tp"),
        P("sp", None),
        P("sp", None),
        P("sp", None, "tp"),
        P("sp", None, "tp"),
        P("sp", "tp", None),
        P("tp", None),
        P("tp", "sp"),
        P("tp", "sp"),
        P("tp", "sp"),
        P("tp", "sp"),
        P("tp", "sp"),
        P(None, "tp", None, None),
        P(None, "tp", None, None),
        P(None, "tp"),
    )
    return jax.shard_map(
        on_device,
        mesh=mesh,
        in_specs=placed,
        out_specs=(
            P("sp", None, "tp"),
            P("sp", None, "tp"),
            P("sp", "tp", None),
            P("sp", "tp"),
            P("tp", "sp"),
            P("tp", "sp"),
            P("tp", "sp"),
        ),
        check_vma=False,
    )
```
